512 devices in a mesh: ep: 32 (over z, x), tp: 16 (over y, core).
Axes of the slice: x: 4, y: 8, z: 8, core: 2. Of those that a mesh axis runs over, the one named last changes fastest.
Arguments:
- queries: bfloat16 [16384, 2048], P('ep', 'tp'), may hold values from -5 to 5
- key_rows: bfloat16 [16384, 2048], P('ep', 'tp'), may hold values from -5 to 5
- values: bfloat16 [16384, 2048], P('ep', 'tp'), may hold values from -6 to 6
- forget_log: float32 [16384, 16], P(None, 'tp'), may hold values from -2051 to 0, as said below
- out_weight: bfloat16 [2048, 4096], P(None, 'tp'), may hold values from -1 to 1
- expert_input: bfloat16 [4096, 4096], P(('ep', 'tp')), may hold values from -6 to 6
- norm_gain: float32 [4096], replicated, may hold values from 0.1 to 1.9
- route_ids: int32 [4096, 2], P('ep'), may hold values from 0 to 31, all different within a row; in each aligned block of 128 rows (0 to 127, 128 to 255, ...) at most 16 rows name the same one
- route_weights: float32 [4096, 2], P('ep'), may hold values from 0.2 to 1
- gate_weight: bfloat16 [32, 4096, 2048], P('ep', None, 'tp'), may hold values from -0.09375 to 0.09375
- up_weight: bfloat16 [32, 4096, 2048], P('ep', None, 'tp'), may hold values from -0.09375 to 0.09375
- down_weight: bfloat16 [32, 2048, 4096], P('ep', None, 'tp'), may hold values from -0.125 to 0.125
Outputs:
- mixer_out: bfloat16 [16384, 4096], P('ep', 'tp')
- expert_out: bfloat16 [4096, 4096], P('ep', 'tp')
The draws below stay inside these ranges and needn't reach their ends.
Inputs may be any that keep to these rules, and one draw needn't show every extreme that they name: forget_log[t, h] is the sum of the log forget gates of head h at positions 0 to t of the one sequence; it never rises along positions. `route_ids`: each row names 2 different experts. In each aligned block of 128 rows (the rows of one index of ep) no expert is named by more than 16 rows, and some block reaches 16.
All inputs are finite; a program needn't handle non-finite values.
Results may differ from the reference program's by a relative error of at most 0.0071.
Values may be sent and summed in bfloat16 or wider, within the bound.
A program may use at most 64 MiB of HBM per device.

```python
import math
import jax
import jax.numpy as jnp
import numpy as np
from jax import lax

D = 4096
HEAD_COUNT = 16
HD = 128
FFE = 2048
TOPK = 2
ROWS_A = 512
ROWS_B = 128
SEQUENCE_LENGTH = 16384
TOKENS_B = 4096
EXPERTS = 32
CAP = 16
N_EP = 32


def draw_queries(key, part):
    drawn_rows = jnp.clip(1.5 * jax.random.normal(jax.random.fold_in(key, 1), (SEQUENCE_LENGTH, HEAD_COUNT * HD), jnp.float32), -5.0, 5.0)
    return drawn_rows.astype(jnp.bfloat16)


def draw_key_rows(key, part):
    drawn_rows = jnp.clip(jax.random.normal(jax.random.fold_in(key, 2), (SEQUENCE_LENGTH, HEAD_COUNT * HD), jnp.float32), -5.0, 5.0)
    return drawn_rows.astype(jnp.bfloat16)


def draw_forget_log(key, part):
    fast_share = 0.5
    fast_heads = jax.random.uniform(jax.random.fold_in(key, 3), (HEAD_COUNT,), jnp.float32) < fast_share
    slow_rate = jnp.exp(jax.random.uniform(jax.random.fold_in(key, 4), (HEAD_COUNT,), jnp.float32, jnp.log(0.2), jnp.log(0.8))) / SEQUENCE_LENGTH
    fast_rate = jnp.exp(jax.random.uniform(jax.random.fold_in(key, 5), (HEAD_COUNT,), jnp.float32, jnp.log(0.01), jnp.log(1.0 / 30.0)))
    head_rate = jnp.where(fast_heads, fast_rate, slow_rate)
    block_factor = jnp.exp(jax.random.uniform(jax.random.fold_in(key, 6), (SEQUENCE_LENGTH // ROWS_A, HEAD_COUNT), jnp.float32, -0.7, 0.7))
    block_factor = jnp.repeat(block_factor, ROWS_A, axis=0)
    roughness = jax.random.uniform(jax.random.fold_in(key, 7), (SEQUENCE_LENGTH, HEAD_COUNT), jnp.float32, 0.3, 1.7)
    step_logarithm = -head_rate[None, :] * block_factor * roughness
    surge_locations = jax.random.randint(jax.random.fold_in(key, 8), (2, HEAD_COUNT), 0, SEQUENCE_LENGTH)
    position_indices = jnp.arange(SEQUENCE_LENGTH, dtype=jnp.int32)
    surge_matched = jnp.any(position_indices[:, None, None] == surge_locations[None, :, :], axis=1)
    surge_penalty = jnp.log(jax.random.uniform(jax.random.fold_in(key, 9), (SEQUENCE_LENGTH, HEAD_COUNT), jnp.float32, 0.6, 0.8))
    step_logarithm = step_logarithm + jnp.where(surge_matched, surge_penalty, 0.0)
    return jnp.cumsum(step_logarithm, axis=0).astype(jnp.float32)


def block_scale(rng, extent, split, least, top_value):
    factor_of, own = 1.0, jax.random.fold_in(rng, 6)
    for dim, shards_of in split:
        draws = jnp.exp(jax.random.uniform(jax.random.fold_in(own, dim), (shards_of,), jnp.float32, least / len(split), top_value / len(split)))
        factor_of = factor_of * jnp.repeat(draws, extent[dim] // shards_of).reshape([-1 if axis == dim else 1 for axis in range(len(extent))])
    return factor_of


def shared_out(rng, own, number, rows, number_of, top, reach, skew):
    order = jax.random.permutation(rng, number_of)
    heavy_load, usual = load_shares(number_of, rows * top, reach, skew, True), load_shares(number_of, rows * top, reach, skew, False)
    places = jnp.arange(number_of)

    def named(sizes, offset_by):
        used = int((sizes > 0).sum())
        fixed = max(1, used // 4)
        passed = fixed + (places - fixed + offset_by * (used - fixed)) % max(1, number_of - fixed)
        return jnp.zeros((number_of,), jnp.int32).at[order[jnp.where(places < fixed, places, passed)]].set(jnp.asarray(sizes, jnp.int32))

    sizes = jnp.where(number % 4 == 0, named(heavy_load, number // 4), named(usual, number - number // 4 - 1))
    mixed = jax.random.permutation(jax.random.fold_in(own, 3), number_of)
    giver, receiver = mixed[0:number_of // 2 * 2:2], mixed[1:number_of // 2 * 2:2]
    slack = jnp.minimum(sizes[giver] - 1, reach - sizes[receiver]) // 2
    slack = jnp.where((giver == order[0]) | (receiver == order[0]) | (sizes[receiver] == 0), 0, jnp.maximum(slack, 0))
    passed = jax.random.randint(jax.random.fold_in(own, 4), (number_of // 2,), 0, 1 << 20) % (slack + 1)
    sizes = sizes.at[giver].add(-passed).at[receiver].add(passed)
    items = jnp.searchsorted(jnp.cumsum(sizes), jnp.arange(rows * top), side="right").astype(jnp.int32)
    table = items.reshape(top, rows).T
    table = table[jax.random.permutation(jax.random.fold_in(own, 1), rows)]
    offset_by = jax.random.randint(jax.random.fold_in(own, 2), (rows, 1), 0, top)
    return jnp.take_along_axis(table, (jnp.arange(top)[None, :] + offset_by) % top, axis=1)


def load_shares(count, total, limit, slope, full):
    portions = [(1 << 20) // math.isqrt(grade ** slope) + 1 for grade in range(1, count + 1)]
    largest = limit if full else min(limit, max(-(-total // count), total * portions[0] // sum(portions)))
    least = 1 if total - largest >= count - 1 else 0
    counts, rest = [largest] + [least] * (count - 1), total - largest - least * (count - 1)
    while rest > 0:
        movable = [i for i in range(1, count) if counts[i] < largest] or [i for i in range(1, count) if counts[i] < limit]
        mass, left = sum([portions[i] for i in movable]), rest
        for i in movable:
            addition = min(limit - counts[i], max(1, left * portions[i] // mass), rest)
            counts[i] = counts[i] + addition
            rest = rest - addition
    return np.array(counts)


def noise(key, dims, width, most, cuts=(), held_as=jnp.bfloat16):
    factor_of = block_scale(key, dims, cuts, -0.22, 0.18) if cuts else 1.0
    drawn = jax.random.normal(key, dims, jnp.float32) * width * factor_of
    return jnp.minimum(jnp.maximum(drawn, -most), most).astype(held_as)


def setup_inputs(seed: int = 0) -> dict:
    key_list = jax.random.split(jax.random.key(seed), 13)
    queries = draw_queries(jax.random.fold_in(key_list[12], 71), 0)
    key_rows = draw_key_rows(jax.random.fold_in(key_list[12], 71), 0)
    values = noise(key_list[2], (SEQUENCE_LENGTH, HEAD_COUNT * HD), 1.0, 6.0, ((0, 32), (1, 16)))
    forget_log = draw_forget_log(jax.random.fold_in(key_list[12], 71), 0)
    out_weight = noise(key_list[4], (HEAD_COUNT * HD, D), (HD // 4) ** -0.5, 1.0, ((1, 16),))
    expert_input = noise(key_list[5], (TOKENS_B, D), 1.0, 6.0, ((0, 512),))
    norm_gain = jnp.clip(1.0 + 0.18 * jax.random.normal(key_list[6], (D,), jnp.float32), 0.1, 1.9)
    route_ids_keys = jax.random.split(jax.random.fold_in(key_list[7], 1), TOKENS_B // ROWS_B)
    route_ids_turns = jax.random.permutation(jax.random.fold_in(key_list[7], 3), TOKENS_B // ROWS_B)
    route_ids = jax.vmap(lambda own, number: shared_out(jax.random.fold_in(key_list[7], 2), own, number, ROWS_B, EXPERTS, TOPK, CAP, 2))(route_ids_keys, route_ids_turns).reshape((TOKENS_B, TOPK))
    route_weights = jnp.clip(0.2 + 0.8 * jax.random.uniform(key_list[8], (TOKENS_B, TOPK), jnp.float32) ** block_scale(key_list[8], (TOKENS_B, TOPK), ((0, 32),), -0.2, 0.2), 0.2, 1.0)
    gate_weight = noise(key_list[9], (EXPERTS, D, FFE), D ** -0.5, 0.09375, ((0, 32), (2, 16)))
    up_weight = noise(key_list[10], (EXPERTS, D, FFE), D ** -0.5, 0.09375, ((0, 32), (2, 16)))
    down_weight = noise(key_list[11], (EXPERTS, FFE, D), FFE ** -0.5, 0.125, ((0, 32), (2, 16)))
    return {"queries": queries, "key_rows": key_rows, "values": values, "forget_log": forget_log, "out_weight": out_weight, "expert_input": expert_input, "norm_gain": norm_gain, "route_ids": route_ids, "route_weights": route_weights, "gate_weight": gate_weight, "up_weight": up_weight, "down_weight": down_weight}


EPSILON = 1e-05

def slot_places(route_rows, experts, capacity):
    entries = route_rows.reshape(-1).astype(jnp.int32)
    matches = (entries[:, None] == jnp.arange(experts, dtype=jnp.int32)[None, :]).astype(jnp.int32)
    earlier = (jnp.cumsum(matches, axis=0) - matches).astype(jnp.int32)
    ranking = lax.optimization_barrier(jnp.sum(earlier * matches, axis=1)).astype(jnp.int32)
    return (entries * capacity + ranking).astype(jnp.int32)

def reference(queries, key_rows, values, forget_log, out_weight, expert_input, norm_gain, route_ids, route_weights, gate_weight, up_weight, down_weight):
    length_all = queries.shape[0]
    query_heads = queries.reshape(length_all, HEAD_COUNT, HD).astype(jnp.float32)
    key_heads = key_rows.reshape(length_all, HEAD_COUNT, HD).astype(jnp.float32)
    value_heads = values.reshape(length_all, HEAD_COUNT, HD).astype(jnp.float32)
    key_places = jnp.arange(length_all, dtype=jnp.int32)
    score_scale = HD ** (-0.5)

    def attend(block_index):
        block_start = (block_index * ROWS_A).astype(jnp.int32)
        query_block = lax.dynamic_slice_in_dim(query_heads, block_start, ROWS_A, 0)
        gate_block = lax.dynamic_slice_in_dim(forget_log, block_start, ROWS_A, 0)
        scores = jnp.einsum('qhd,khd->hqk', query_block, key_heads) * score_scale
        scores = scores + gate_block.T[:, :, None] - forget_log.T[:, None, :]
        query_places = block_start + jnp.arange(ROWS_A, dtype=jnp.int32)
        scores = jnp.where(key_places[None, None, :] <= query_places[None, :, None], scores, -jnp.inf)
        row_max = lax.optimization_barrier(jnp.max(scores, axis=2, keepdims=True))
        weights_now = jnp.exp(scores - row_max)
        denominator = lax.optimization_barrier(jnp.sum(weights_now, axis=2))
        rounded = lax.optimization_barrier(weights_now.astype(jnp.bfloat16)).astype(jnp.float32)
        numerator = jnp.einsum('hqk,khd->qhd', rounded, value_heads)
        return (numerator / denominator.T[:, :, None]).astype(jnp.bfloat16)
    attended = lax.map(attend, jnp.arange(length_all // ROWS_A, dtype=jnp.int32)).reshape(length_all, HEAD_COUNT * HD)
    mixer_out = jnp.dot(attended, out_weight, preferred_element_type=jnp.float32).astype(jnp.bfloat16)
    as_float = expert_input.astype(jnp.float32)
    center = lax.optimization_barrier(jnp.mean(as_float, axis=1, keepdims=True))
    variance = lax.optimization_barrier(jnp.mean(jnp.square(as_float - center), axis=1, keepdims=True))
    normed = ((as_float - center) * lax.rsqrt(variance + EPSILON) * norm_gain).astype(jnp.bfloat16)
    blocks = route_ids.reshape(N_EP, ROWS_B, TOPK)
    places = jax.vmap(lambda block_ids: slot_places(block_ids, EXPERTS, CAP))(blocks)
    expert_of = blocks.reshape(N_EP, ROWS_B * TOPK).astype(jnp.int32)
    ranking = places - expert_of * CAP
    block_index = jnp.arange(N_EP, dtype=jnp.int32)[:, None]
    global_slot = (expert_of * (N_EP * CAP) + block_index * CAP + ranking).astype(jnp.int32)
    owners = (block_index * ROWS_B + jnp.arange(ROWS_B * TOPK, dtype=jnp.int32)[None, :] // TOPK).astype(jnp.int32)
    slot_table = jnp.full((EXPERTS * N_EP * CAP,), TOKENS_B, jnp.int32).at[global_slot.reshape(-1)].set(owners.reshape(-1))
    slot_table = slot_table.reshape(EXPERTS, N_EP * CAP)

    def run_expert(expert_index):
        chosen_rows = jnp.take(normed, slot_table[expert_index], axis=0, mode='fill', fill_value=0)
        gate_part = jnp.dot(chosen_rows, gate_weight[expert_index], preferred_element_type=jnp.float32)
        up_part = jnp.dot(chosen_rows, up_weight[expert_index], preferred_element_type=jnp.float32)
        hidden = (jax.nn.silu(gate_part) * up_part).astype(jnp.bfloat16)
        return jnp.dot(hidden, down_weight[expert_index], preferred_element_type=jnp.float32).astype(jnp.bfloat16)
    results = lax.map(run_expert, jnp.arange(EXPERTS, dtype=jnp.int32)).reshape(EXPERTS * N_EP * CAP, D)
    picked = jnp.take(results, global_slot.reshape(-1), axis=0).astype(jnp.float32)
    combined = lax.optimization_barrier(jnp.sum((picked * route_weights.reshape(-1)[:, None]).reshape(TOKENS_B, TOPK, D), axis=1))
    return (mixer_out, combined.astype(jnp.bfloat16))
```

```python
import math

import jax
import jax.numpy as jnp
from jax import lax
from jax.experimental import pallas as pl
from jax.experimental.pallas import tpu as pltpu
from jax.sharding import PartitionSpec as P

MESH = pl.DeviceIdType.MESH
EPSILON = 1e-05
LOG2E = math.log2(math.e)
LOW = -1e30
NT = (((1,), (1,)), ((), ()))
NN = (((1,), (0,)), ((), ()))
TN = (((0,), (0,)), ((), ()))
F32 = jnp.float32
BF16 = jnp.bfloat16

NX, NZ, NE = 4, 8, 32
NY, NTP = 8, 16
ROWS, HD, D = 512, 128, 4096
CAP, TOK, WIDE = 16, 128, 256
SLOTS = NE * CAP
GROUP = NX * ROWS


def dot(a, b, dims):
    return lax.dot_general(a, b, dims, preferred_element_type=F32)


def kernel(
    q_ref, k_ref, v_ref, fl_ref, xin_ref, gain_ref, ids_ref, rw_ref,
    gate_hbm, up_hbm, down_hbm, out_hbm,
    mix_ref, exp_ref,
    k4, vt4, q8, bias, po_out, ps_out, po_in, ps_in, m_s, l_s, acc_s, num_s, den_s, top_s,
    xs, tok, disp, gath, accg, hb, accd, res, ret, ab, accm,
    wgu, wd, wo,
    w_sem, kv_send, kv_recv, q_send, q_recv, tok_send, tok_recv, d_send, d_recv,
    po_send, po_recv, ps_send, ps_recv,
    g_send, g_recv, h_send, h_recv, a_send, a_recv, b_send, b_recv,
):
    e = lax.axis_index("ep")
    t = lax.axis_index("tp")
    z, x = lax.div(e, NX), lax.rem(e, NX)
    y, c = lax.div(t, 2), lax.rem(t, 2)

    def remote(src, dst, ssem, rsem, ep, tp):
        return pltpu.make_async_remote_copy(
            src_ref=src, dst_ref=dst, send_sem=ssem, recv_sem=rsem,
            device_id=(ep, tp), device_id_type=MESH,
        )

    def each(low, high, fn):
        def step(i, carry):
            fn(i)
            return carry
        lax.fori_loop(low, high, step, 0)

    weights = (
        pltpu.make_async_copy(gate_hbm, wgu.at[:, pl.ds(0, 128)], w_sem.at[0]),
        pltpu.make_async_copy(up_hbm, wgu.at[:, pl.ds(128, 128)], w_sem.at[1]),
        pltpu.make_async_copy(down_hbm, wd, w_sem.at[2]),
        pltpu.make_async_copy(out_hbm, wo, w_sem.at[3]),
    )
    for copy in weights:
        copy.start()

    barrier = pltpu.get_barrier_semaphore()

    def greet_ep(i):
        pl.semaphore_signal(
            barrier, inc=1, device_id=(lax.rem(e + i, NE), t), device_id_type=MESH
        )

    def greet_tp(i):
        pl.semaphore_signal(
            barrier, inc=1, device_id=(e, lax.rem(t + i, NTP)), device_id_type=MESH
        )

    each(1, NE, greet_ep)
    each(1, NTP, greet_tp)

    rows = xin_ref[...].astype(F32)
    center = jnp.mean(rows, axis=1, keepdims=True)
    spread = rows - center
    variance = jnp.mean(spread * spread, axis=1, keepdims=True)
    normed = (spread * lax.rsqrt(variance + EPSILON) * gain_ref[...]).astype(BF16).astype(F32)
    for i in range(NTP):
        xs[i] = normed[:, WIDE * i : WIDE * (i + 1)]
    tok[t] = xs[t]
    k4[x] = k_ref[...]
    vt4[x] = v_ref[...].astype(F32).T.astype(BF16)
    q8[z] = q_ref[...]

    ids = ids_ref[...]
    experts = lax.broadcasted_iota(jnp.int32, (NE, TOK), 0)
    match = [(experts == ids[i : i + 1, :]).astype(F32) for i in range(2)]
    before = (
        lax.broadcasted_iota(jnp.int32, (TOK, TOK), 0)
        < lax.broadcasted_iota(jnp.int32, (TOK, TOK), 1)
    ).astype(F32).astype(BF16)
    earlier = dot((match[0] + match[1]).astype(BF16), before, NN)
    slot_rows = lax.broadcasted_iota(jnp.int32, (SLOTS, TOK), 0)
    places = [
        ids[i : i + 1, :] * CAP
        + jnp.sum(earlier * match[i], axis=0, keepdims=True).astype(jnp.int32)
        for i in range(2)
    ]

    def picks(i):
        return (slot_rows == places[i]).astype(F32)

    pl.semaphore_wait(barrier, NE + NTP - 2)

    def tok_copy(i, peer):
        return remote(xs.at[peer], tok.at[t], tok_send.at[i], tok_recv.at[t], e, peer)

    each(1, NTP, lambda i: tok_copy(i, lax.rem(t + i, NTP)).start())

    def kv_copies(i):
        peer = z * NX + lax.rem(x + i, NX)
        return (
            remote(k4.at[x], k4.at[x], kv_send.at[i], kv_recv.at[x], peer, t),
            remote(vt4.at[x], vt4.at[x], kv_send.at[NX + i], kv_recv.at[NX + x], peer, t),
        )

    for i in range(1, NX):
        for copy in kv_copies(i):
            copy.start()

    def tok_arrive(i):
        src = lax.rem(t + i, NTP)
        remote(xs.at[src], tok.at[src], tok_send.at[i], tok_recv.at[src], e, src).wait_recv()

    each(1, NTP, tok_arrive)
    routed = (picks(0) + picks(1)).astype(BF16)
    tokens = tok[...].reshape(TOK, WIDE).astype(BF16)
    disp[...] = dot(routed, tokens, NN).astype(BF16).reshape(NE, CAP, WIDE)
    gath[t, e] = disp[e]

    def d_copy(i):
        peer = lax.rem(e + i, NE)
        return remote(disp.at[peer], gath.at[t, e], d_send.at[i], d_recv.at[e], peer, t)

    each(1, NE, lambda i: d_copy(i).start())

    def q_copy(zz):
        return remote(q8.at[z], q8.at[z], q_send.at[zz], q_recv.at[z], zz * NX + x, t)

    each(0, z, lambda i: q_copy(z - 1 - i).start())

    key_row = fl_ref[:, pl.ds(pl.multiple_of(z * GROUP, GROUP), GROUP)]
    base = key_row[:, 0:1]
    bias_row = (base - key_row) * LOG2E
    for i in range(GROUP // 128):
        piece = bias_row[:, 128 * i : 128 * (i + 1)]
        bias[pl.ds(128 * i, 128), :] = jnp.broadcast_to(piece, (128, 128)).T

    for i in range(1, NX):
        src = lax.rem(x + i, NX)
        remote(k4.at[src], k4.at[src], kv_send.at[i], kv_recv.at[src], e, t).wait_recv()
        remote(vt4.at[src], vt4.at[src], kv_send.at[i], kv_recv.at[NX + src], e, t).wait_recv()

    unit_scale = LOG2E * HD ** (-0.5)

    def logits(b, queries):
        shift = bias[pl.ds(ROWS * b, ROWS), :]
        shift = jnp.concatenate([shift, shift], axis=1)
        return dot(k4[b], queries, NT) * unit_scale + shift

    def query_shift(k, h):
        start = pl.multiple_of((x + NX * k) * ROWS + WIDE * h, WIDE)
        return (fl_ref[:, pl.ds(start, WIDE)] - base) * LOG2E

    def fold(state, b, scores):
        top, total, acc = state
        newest = jnp.maximum(top, jnp.max(scores, axis=0, keepdims=True))
        factor = jnp.exp2(top - newest)
        weights_now = jnp.exp2(scores - newest)
        total = total * factor + jnp.sum(weights_now, axis=0, keepdims=True)
        acc = acc * factor + dot(vt4[b], weights_now.astype(BF16), NN)
        return newest, total, acc

    def fresh():
        return (
            jnp.full((1, WIDE), LOW, F32),
            jnp.zeros((1, WIDE), F32),
            jnp.zeros((HD, WIDE), F32),
        )

    for h in range(2):
        lanes = pl.ds(WIDE * h, WIDE)
        m_s[...], l_s[...], acc_s[...] = fresh()
        ahead = lax.broadcasted_iota(jnp.int32, (ROWS, WIDE), 0) - lax.broadcasted_iota(
            jnp.int32, (ROWS, WIDE), 1
        )

        def chunk(b):
            scores = logits(b, q8[z, pl.ds(WIDE * h, WIDE), :])
            scores = jnp.where(ahead <= WIDE * h + ROWS * (x - b), scores, LOW)
            m_s[...], l_s[...], acc_s[...] = fold((m_s[...], l_s[...], acc_s[...]), b, scores)

        each(0, x + 1, chunk)
        num_s[:, lanes] = acc_s[...] / l_s[...]
        top_s[:, lanes] = m_s[...] + jnp.log2(l_s[...]) + query_shift(z, h)
        den_s[:, lanes] = jnp.ones((1, WIDE), F32)

    def po_copies(k):
        return (
            remote(po_out.at[k], po_in.at[z], po_send.at[k], po_recv.at[z], k * NX + x, t),
            remote(ps_out.at[k], ps_in.at[z], ps_send.at[k], ps_recv.at[z], k * NX + x, t),
        )

    def unit(k):
        remote(q8.at[k], q8.at[k], q_send.at[k], q_recv.at[k], e, t).wait_recv()
        for h in range(2):
            queries = q8[k, pl.ds(WIDE * h, WIDE), :]
            state = fresh()
            for b in range(NX):
                state = fold(state, b, logits(b, queries))
            top, total, acc = state
            po_out[k, :, pl.ds(WIDE * h, WIDE)] = (acc / total).astype(BF16)
            ps_out[k, :, pl.ds(WIDE * h, WIDE)] = top + jnp.log2(total) + query_shift(k, h)
        for copy in po_copies(k):
            copy.start()

    def units(first, last):
        each(jnp.minimum(z + first, NZ), jnp.minimum(z + last, NZ), unit)

    def ring(buf, ssem, rsem, half, consume, between):
        right, left = 2 * lax.rem(y + 1, NY) + c, 2 * lax.rem(y + NY - 1, NY) + c
        other = 1 - 2 * c
        started = []

        def copy(src, i, r, tp):
            return remote(src, src, ssem.at[i], rsem.at[r], e, tp)

        def send(src, r, tp):
            one = copy(src, len(started), r, tp)
            one.start()
            started.append(one)

        def arrive(src, r):
            copy(src, 0, r, right).wait_recv()

        def slot_of(step):
            return 2 * lax.rem(y + step + NY, NY) + c

        near = pl.ds(0, half)
        far = pl.ds(half, half)
        send(buf.at[t], t, right)
        send(buf.at[t], t, left)
        send(buf.at[t], t, t + other)
        consume(t)
        earlier_slots = [t]
        for s in range(1, 4):
            a, b = slot_of(-s), slot_of(s)
            arrive(buf.at[a], a)
            send(buf.at[a] if s < 3 else buf.at[a, near], a if s < 3 else NTP, right)
            send(buf.at[a], a, t + other)
            arrive(buf.at[b], b)
            send(buf.at[b] if s < 3 else buf.at[b, far], b if s < 3 else NTP + 1, left)
            send(buf.at[b], b, t + other)
            between(s)
            consume(a)
            consume(b)
            for slot in earlier_slots:
                arrive(buf.at[slot + other], slot + other)
                consume(slot + other)
            earlier_slots = [a, b]
        a = slot_of(4)
        arrive(buf.at[a, near], NTP)
        arrive(buf.at[a, far], NTP + 1)
        send(buf.at[a], a, t + other)
        between(4)
        consume(a)
        for slot in earlier_slots + [a]:
            arrive(buf.at[slot + other], slot + other)
            consume(slot + other)
        return started

    for copy in weights:
        copy.wait()

    def d_arrive(i):
        src = lax.rem(e + i, NE)
        remote(disp.at[src], gath.at[t, src], d_send.at[i], d_recv.at[src], src, t).wait_recv()

    each(1, NE, d_arrive)

    accg[...] = jnp.zeros_like(accg)

    def gate_up(slot):
        part = wgu[pl.ds(pl.multiple_of(slot * WIDE, WIDE), WIDE), :]
        accg[...] += dot(gath[slot].reshape(SLOTS, WIDE), part, NN)

    spans = {1: (1, 3), 2: (3, 5), 3: (5, 7), 4: (7, 8)}
    started = ring(gath, g_send, g_recv, NE // 2, gate_up, lambda s: units(*spans[s]))
    gate = accg[:, 0:128]
    hb[t] = (gate / (1.0 + jnp.exp(-gate)) * accg[:, 128:256]).astype(BF16)

    accd[...] = jnp.zeros_like(accd)

    def down(slot):
        part = wd[pl.ds(pl.multiple_of(slot * 128, 128), 128), :]
        accd[...] += dot(hb[slot], part, NN)

    started += ring(hb, h_send, h_recv, SLOTS // 2, down, lambda s: None)
    res[...] = accd[...].astype(BF16).reshape(NE, CAP, WIDE)
    ret[e] = res[e]

    def b_copy(i):
        peer = lax.rem(e + i, NE)
        return remote(res.at[peer], ret.at[e], b_send.at[i], b_recv.at[e], peer, t)

    each(1, NE, lambda i: b_copy(i).start())

    def merge(i):
        zz = z - 1 - i
        remote(po_out.at[zz], po_in.at[zz], po_send.at[zz], po_recv.at[zz], e, t).wait_recv()
        remote(ps_out.at[zz], ps_in.at[zz], ps_send.at[zz], ps_recv.at[zz], e, t).wait_recv()
        top, new = top_s[...], ps_in[zz]
        newest = jnp.maximum(top, new)
        keep, add = jnp.exp2(top - newest), jnp.exp2(new - newest)
        top_s[...] = newest
        den_s[...] = den_s[...] * keep + add
        num_s[...] = num_s[...] * keep + po_in[zz].astype(F32) * add

    each(0, z, merge)
    ab[t] = (num_s[...] / den_s[...]).astype(BF16)
    accm[...] = jnp.zeros_like(accm)

    def project(slot):
        part = wo[pl.ds(pl.multiple_of(slot * HD, HD), HD), :]
        accm[...] += dot(ab[slot], part, TN)

    started += ring(ab, a_send, a_recv, HD // 2, project, lambda s: None)
    mix_ref[...] = accm[...].astype(BF16)

    def b_arrive(i):
        src = lax.rem(e + i, NE)
        remote(res.at[src], ret.at[src], b_send.at[i], b_recv.at[src], src, t).wait_recv()

    each(1, NE, b_arrive)
    back = ret[...].reshape(SLOTS, WIDE)
    square = lax.broadcasted_iota(jnp.int32, (TOK, TOK), 0) == lax.broadcasted_iota(
        jnp.int32, (TOK, TOK), 1
    )
    total = jnp.zeros((TOK, WIDE), F32)
    for i in range(2):
        scale = jnp.sum(
            jnp.where(square, rw_ref[i : i + 1, :], 0.0), axis=1, keepdims=True
        )
        total = total + dot(picks(i).astype(BF16), back, TN) * scale
    exp_ref[...] = total.astype(BF16)

    for copy in started:
        copy.wait_send()
    each(1, NTP, lambda i: tok_copy(i, lax.rem(t + i, NTP)).wait_send())
    for i in range(1, NX):
        for copy in kv_copies(i):
            copy.wait_send()
    each(1, NE, lambda i: d_copy(i).wait_send())
    each(0, z, lambda i: q_copy(i).wait_send())
    each(1, NE, lambda i: b_copy(i).wait_send())

    def po_sent(k):
        for copy in po_copies(k):
            copy.wait_send()

    each(z + 1, NZ, po_sent)


def body(
    queries, key_rows, values, forget_log, out_weight, expert_input, norm_gain,
    route_ids, route_weights, gate_weight, up_weight, down_weight,
):
    vmem = pl.BlockSpec(memory_space=pltpu.VMEM)
    hbm = pl.BlockSpec(memory_space=pl.ANY)
    dma = pltpu.SemaphoreType.DMA
    return pl.pallas_call(
        kernel,
        out_shape=(
            jax.ShapeDtypeStruct((ROWS, WIDE), BF16),
            jax.ShapeDtypeStruct((TOK, WIDE), BF16),
        ),
        in_specs=[vmem] * 8 + [hbm] * 4,
        out_specs=(vmem, vmem),
        scratch_shapes=[
            pltpu.VMEM((NX, ROWS, HD), BF16),
            pltpu.VMEM((NX, HD, ROWS), BF16),
            pltpu.VMEM((NZ, ROWS, HD), BF16),
            pltpu.VMEM((GROUP, 128), F32),
            pltpu.VMEM((NZ, HD, ROWS), BF16),
            pltpu.VMEM((NZ, 1, ROWS), F32),
            pltpu.VMEM((NZ, HD, ROWS), BF16),
            pltpu.VMEM((NZ, 1, ROWS), F32),
            pltpu.VMEM((1, WIDE), F32),
            pltpu.VMEM((1, WIDE), F32),
            pltpu.VMEM((HD, WIDE), F32),
            pltpu.VMEM((HD, ROWS), F32),
            pltpu.VMEM((1, ROWS), F32),
            pltpu.VMEM((1, ROWS), F32),
            pltpu.VMEM((NTP, 8, WIDE), F32),
            pltpu.VMEM((NTP, 8, WIDE), F32),
            pltpu.VMEM((NE, CAP, WIDE), BF16),
            pltpu.VMEM((NTP, NE, CAP, WIDE), BF16),
            pltpu.VMEM((SLOTS, WIDE), F32),
            pltpu.VMEM((NTP, SLOTS, 128), BF16),
            pltpu.VMEM((SLOTS, WIDE), F32),
            pltpu.VMEM((NE, CAP, WIDE), BF16),
            pltpu.VMEM((NE, CAP, WIDE), BF16),
            pltpu.VMEM((NTP, HD, ROWS), BF16),
            pltpu.VMEM((ROWS, WIDE), F32),
            pltpu.VMEM((D, 256), BF16),
            pltpu.VMEM((2048, WIDE), BF16),
            pltpu.VMEM((2048, WIDE), BF16),
            dma((4,)),
            dma((2 * NX,)), dma((2 * NX,)),
            dma((NZ,)), dma((NZ,)),
            dma((NTP,)), dma((NTP,)),
            dma((NE,)), dma((NE,)),
            dma((NZ,)), dma((NZ,)), dma((NZ,)), dma((NZ,)),
            dma((16,)), dma((NTP + 2,)),
            dma((16,)), dma((NTP + 2,)),
            dma((16,)), dma((NTP + 2,)),
            dma((NE,)), dma((NE,)),
        ],
        compiler_params=pltpu.CompilerParams(
            collective_id=0, has_side_effects=True, vmem_limit_bytes=56 * 1024 * 1024
        ),
    )(
        queries, key_rows, values, forget_log.reshape(1, -1), expert_input,
        norm_gain.reshape(1, -1), route_ids.T, route_weights.T,
        gate_weight.reshape(D, 128), up_weight.reshape(D, 128),
        down_weight.reshape(2048, WIDE), out_weight,
    )


def solution(mesh):
    placed = (
        P("ep", "tp"), P("ep", "tp"), P("ep", "tp"), P(None, "tp"), P(None, "tp"),
        P(("ep", "tp"), None), P(), P("ep", None), P("ep", None),
        P("ep", None, "tp"), P("ep", None, "tp"), P("ep", None, "tp"),
    )
    return jax.shard_map(
        body, mesh=mesh, in_specs=placed, out_specs=(P("ep", "tp"), P("ep", "tp")),
        check_vma=False,
    )
```
